1024 devices in a mesh: ra: 128 (over z, y), cb: 8 (over x, core).
Axes of the slice: x: 4, y: 8, z: 16, core: 2. Of those that a mesh axis runs over, the one named last changes fastest.
Arguments:
- tokens: bfloat16 [512, 4096], P(None, 'cb'), may hold values from -400 to 400
- norm_gain: bfloat16 [4096], P('cb'), may hold values from 0.099609375 to 1.8984375
- w_gate: bfloat16 [4096, 11264], P('cb', 'ra'), may hold values from -0.09375 to 0.09375
- w_up: bfloat16 [4096, 11264], P('cb', 'ra'), may hold values from -0.09375 to 0.09375
- w_down: bfloat16 [11264, 4096], P('ra', 'cb'), may hold values from -0.0546875 to 0.0546875
- out_gain: bfloat16 [4096], P('cb'), may hold values from 0.099609375 to 1.8984375
Outputs:
- normed_out: bfloat16 [512, 4096], P('ra', 'cb')
The draws below stay inside these ranges and needn't reach their ends.
All inputs are finite; a program needn't handle non-finite values.
Results may differ from the reference program's by a relative error of at most 0.0045.
Values sent between devices are 32-bit elements; how exact they have to be, the bound alone decides.
No kernel may reach another device: no remote copies, remote signals or barrier semaphores. Data moves between devices by JAX's collectives and lax.ppermute only.
A program may use at most 32 MiB of HBM per device.

```python
import jax
import jax.numpy as jnp
from jax import lax

D = 4096
FF = 11264
TOKENS = 512


def draw_tokens(key, part):
    first, second, third = jax.random.split(jax.random.fold_in(key, 17), 3)
    rise = jnp.arange(D, dtype=jnp.float32) / D
    jitter = jax.random.uniform(second, (D,), jnp.float32)
    column_scale = jnp.exp(jnp.log(10.0) * (0.8 * rise + 0.2 * jitter))
    row_scale = jnp.exp(jnp.log(10.0) * jax.random.uniform(third, (TOKENS, 1), jnp.float32))
    base = jnp.clip(jax.random.normal(first, (TOKENS, D), jnp.float32), -4.0, 4.0)
    return (base * row_scale * column_scale[None, :]).astype(jnp.bfloat16)


def level_of(stream_key, dims, cuts, least, largest):
    gain, own = 1.0, jax.random.fold_in(stream_key, 6)
    for dim, parts in cuts:
        draws = jnp.exp(jax.random.uniform(jax.random.fold_in(own, dim), (parts,), jnp.float32, least / len(cuts), largest / len(cuts)))
        gain = gain * jnp.repeat(draws, dims[dim] // parts).reshape([-1 if axis == dim else 1 for axis in range(len(dims))])
    return gain


def scatter_about(rng, shape, deviation, most, shards=(), held_as=jnp.bfloat16):
    loudness = level_of(rng, shape, shards, -0.22, 0.18) if shards else 1.0
    drawn = jax.random.normal(rng, shape, jnp.float32) * deviation * loudness
    return jnp.minimum(jnp.maximum(drawn, -most), most).astype(held_as)


def setup_inputs(seed: int = 0) -> dict:
    keys = jax.random.split(jax.random.key(seed), 7)
    return {
        "tokens": draw_tokens(jax.random.fold_in(keys[6], 71), 0),
        "norm_gain": jnp.clip(1.0 + 0.18 * jax.random.normal(keys[1], (D,), jnp.float32), 0.099609375, 1.8984375).astype(jnp.bfloat16),
        "w_gate": scatter_about(keys[2], (D, FF), D ** -0.5, 0.09375, ((0, 8), (1, 128))),
        "w_up": scatter_about(keys[3], (D, FF), D ** -0.5, 0.09375, ((0, 8), (1, 128))),
        "w_down": scatter_about(keys[4], (FF, D), FF ** -0.5, 0.0546875, ((0, 128), (1, 8))),
        "out_gain": jnp.clip(1.0 + 0.18 * jax.random.normal(keys[5], (D,), jnp.float32), 0.099609375, 1.8984375).astype(jnp.bfloat16),
    }


def reference(tokens, norm_gain, w_gate, w_up, w_down, out_gain):
    eps = 1e-06
    xfloat = tokens.astype(jnp.float32)
    inv_in = lax.rsqrt(lax.optimization_barrier(jnp.mean(xfloat * xfloat, axis=1, keepdims=True)) + eps)
    scaled = (xfloat * norm_gain.astype(jnp.float32)).astype(jnp.bfloat16)
    gate = jnp.dot(scaled, w_gate, preferred_element_type=jnp.float32) * inv_in
    up = jnp.dot(scaled, w_up, preferred_element_type=jnp.float32) * inv_in
    hidden = (jax.nn.silu(gate) * up).astype(jnp.bfloat16)
    down = jnp.dot(hidden, w_down, preferred_element_type=jnp.float32)
    mixed = 0.1 * xfloat + down
    inv_out = lax.rsqrt(lax.optimization_barrier(jnp.mean(mixed * mixed, axis=1, keepdims=True)) + eps)
    return (mixed * inv_out * out_gain.astype(jnp.float32)).astype(jnp.bfloat16)
```

```python
import jax
import jax.numpy as jnp
from jax import lax
from jax.experimental import pallas as pl
from jax.experimental.pallas import tpu as pltpu
from jax.sharding import Mesh
from jax.sharding import PartitionSpec as P

D = 4096
EPS = 1e-06
RA = ("zq", "z0", "yq", "y0")
QUAD = ("z0", "y0")
REST = ("zq", "yq")
NT = (((1,), (1,)), ((), ()))
F32 = jnp.float32
BF16 = jnp.bfloat16
SMALL = pltpu.CompilerParams(vmem_limit_bytes=8 * 1024 * 1024)


def exchange(array, axes):
    return lax.all_to_all(array, axes, split_axis=0, concat_axis=0, tiled=True)


def front(tok, gain, wg, wu, out):
    x = tok[...].astype(F32)
    sq = jnp.sum(x * x, axis=1, keepdims=True)
    scaled = (x * gain[...].astype(F32)).astype(BF16)
    g = lax.dot_general(scaled, wg[...], NT, preferred_element_type=F32)
    u = lax.dot_general(scaled, wu[...], NT, preferred_element_type=F32)
    rows, units = g.shape
    fill = jnp.broadcast_to(sq, (rows, 128 - units))
    out[...] = jnp.concatenate([g, fill, u, fill], axis=1)


def middle(parts, out):
    n_z0, n_y0, n_cb, held, units = out.shape
    total = jnp.sum(parts[...], axis=0)
    inv = lax.rsqrt(total[:, units : units + 1] / D + EPS)
    g = total[:, :units] * inv
    u = total[:, 128 : 128 + units] * inv
    hidden = (g / (1.0 + jnp.exp(-g)) * u).astype(BF16).astype(F32)
    r = 4
    n_yq = held // r
    for a in range(n_z0):
        for b in range(n_y0):
            rows = [((a * n_yq + q) * n_y0 + b) * r for q in range(n_yq)]
            block = jnp.concatenate([hidden[s : s + r] for s in rows], axis=0)
            for j in range(n_cb):
                out[a, b, j] = block


def back(me, hid, w0, w1, w2, w3, out):
    acc = None
    for k, w in enumerate((w0, w1, w2, w3)):
        left = hid[me[0] ^ k].astype(BF16)
        part = jnp.dot(left, w[...].astype(BF16), preferred_element_type=F32)
        acc = part if acc is None else acc + part
    n, per, _ = out.shape
    for k in range(n):
        out[k] = acc[k * per : (k + 1) * per]


def fold(row, sums, tok, mixed, sq):
    n, per, _ = sums.shape
    down = jnp.sum(sums[...], axis=0)
    pair = tok[...].astype(F32)
    residual = jnp.where(row[0] % 2 == 1, pair[per:], pair[:per])
    value = 0.1 * residual + down
    mixed[...] = value
    total = jnp.sum(value * value, axis=1, keepdims=True)
    sq[...] = jnp.broadcast_to(total[None], sq.shape)


def finish(mixed, sq, gain, out):
    total = jnp.sum(sq[...], axis=0)[:, :1]
    inv = lax.rsqrt(total / D + EPS)
    out[...] = (mixed[...] * inv * gain[...].astype(F32)).astype(BF16)


def body(tokens, norm_gain, w_gate, w_up, w_down, out_gain):
    n_cb = lax.axis_size("cb")
    n_quad = lax.axis_size(QUAD)
    n_rest = lax.axis_size(REST)
    rows, cols = tokens.shape
    units = w_gate.shape[1]
    own = rows // lax.axis_size(RA)
    share = rows // n_cb
    held = share // n_quad

    mine = w_down.astype(F32)
    others = []
    for k in range(1, n_quad):
        with jax.named_scope(f"weights{k}"):
            others.append(lax.ppermute(mine, QUAD, [(i, i ^ k) for i in range(n_quad)]))

    partial = pl.pallas_call(front, out_shape=jax.ShapeDtypeStruct((rows, 256), F32), name="front", compiler_params=SMALL)(
        tokens, norm_gain[None, :], w_gate.T, w_up.T)
    with jax.named_scope("parts"):
        parts = exchange(partial.reshape(n_cb, share, 256), "cb")
    with jax.named_scope("gating"):
        blocks = pl.pallas_call(middle, out_shape=jax.ShapeDtypeStruct((2, 2, n_cb, held, units), F32), name="middle", compiler_params=SMALL)(parts)
    with jax.named_scope("spread"):
        got = exchange(blocks.reshape(n_quad * n_cb, held, units), QUAD + ("cb",))

    me = lax.axis_index(QUAD).astype(jnp.int32)[None]
    sums = pl.pallas_call(
        back,
        grid_spec=pltpu.PrefetchScalarGridSpec(num_scalar_prefetch=1, grid=(1,), in_specs=[
            pl.BlockSpec((n_quad, n_cb * held, units), lambda i, m: (0, 0, 0)),
            *[pl.BlockSpec((units, cols), lambda i, m: (0, 0))] * 4,
        ], out_specs=pl.BlockSpec((n_rest, own, cols), lambda i, m: (0, 0, 0))),
        out_shape=jax.ShapeDtypeStruct((n_rest, own, cols), F32), name="back", compiler_params=SMALL)(
        me, got.reshape(n_quad, n_cb * held, units), w_down, *others)
    with jax.named_scope("scatter"):
        sums = exchange(sums, REST)

    row = lax.axis_index(RA).astype(jnp.int32)[None]
    mixed, sq = pl.pallas_call(
        fold,
        grid_spec=pltpu.PrefetchScalarGridSpec(num_scalar_prefetch=1, grid=(1,), in_specs=[
            pl.BlockSpec((n_rest, own, cols), lambda i, m: (0, 0, 0)),
            pl.BlockSpec((2 * own, cols), lambda i, m: (m[0] // 2, 0)),
        ], out_specs=[pl.BlockSpec((own, cols), lambda i, m: (0, 0)), pl.BlockSpec((n_cb, own, 128), lambda i, m: (0, 0, 0))]),
        out_shape=[jax.ShapeDtypeStruct((own, cols), F32), jax.ShapeDtypeStruct((n_cb, own, 128), F32)], name="fold", compiler_params=SMALL)(
        row, sums, tokens)
    with jax.named_scope("norm"):
        sq = exchange(sq, "cb")
    return pl.pallas_call(finish, out_shape=jax.ShapeDtypeStruct((own, cols), BF16), name="finish", compiler_params=SMALL)(
        mixed, sq, out_gain[None, :])


def solution(mesh):
    finer = Mesh(mesh.devices.reshape(8, 2, 4, 2, mesh.shape["cb"]), (*RA, "cb"))
    placed = (P(None, "cb"), P("cb"), P("cb", RA), P("cb", RA), P(RA, "cb"), P("cb"))
    return jax.shard_map(body, mesh=finer, in_specs=placed, out_specs=P(RA, "cb"), check_vma=False)
```

```python
import jax
import jax.numpy as jnp
from jax import lax
from jax.experimental import pallas as pl
from jax.experimental.pallas import tpu as pltpu
from jax.sharding import Mesh
from jax.sharding import PartitionSpec as P


D = 4096
EPS = 1e-06
RA = ("zq", "z0", "yq", "y0")
QUAD = ("z0", "y0")
REST = ("zq", "yq")
NT = (((1,), (1,)), ((), ()))
F32 = jnp.float32
BF16 = jnp.bfloat16
SMALL = pltpu.CompilerParams(vmem_limit_bytes=8 * 1024 * 1024)


def exchange(array, axes):
    return lax.all_to_all(array, axes, split_axis=0, concat_axis=0, tiled=True)


def copies(sources, targets, sems):
    started = [pltpu.make_async_copy(s, t, sems.at[k]) for k, (s, t) in enumerate(zip(sources, targets))]
    for c in started:
        c.start()
    return started


def front(tok_hbm, gain_hbm, wg_hbm, wu_hbm, out, tok, gain, wg, wu, sems):
    pending = copies((tok_hbm, gain_hbm, wg_hbm, wu_hbm), (tok, gain, wg, wu), sems)
    n_cb, _, lanes = out.shape
    rows, cols = tok.shape
    units = wg.shape[0]
    share = rows // n_cb
    half = share // 2
    first = lanes - units
    pending[0].wait()
    pending[1].wait()
    x = tok[...].astype(F32)
    sq = jnp.sum(x * x, axis=1, keepdims=True)
    scaled = (x * gain[...].astype(F32).reshape(1, cols)).astype(BF16)
    pending[2].wait()
    pending[3].wait()
    up = wu[...].astype(F32)
    left = jnp.concatenate([wg[...].astype(F32), up[:first]], axis=0).astype(BF16)
    gap = jnp.zeros((lanes // 2 - (units - first), cols), F32)
    none = jnp.zeros((lanes // 2, cols), F32)
    low = jnp.concatenate([up[first:], gap, none], axis=0).astype(BF16)
    high = jnp.concatenate([none, up[first:], gap], axis=0).astype(BF16)
    main = lax.dot_general(scaled, left, NT, preferred_element_type=F32)
    blocks = scaled.reshape(n_cb, 2, half, cols)
    sums = sq.reshape(n_cb, 2, half, 1)
    lane = lax.broadcasted_iota(jnp.int32, (n_cb * half, lanes), 1)
    rest = lax.dot_general(blocks[:, 0].reshape(n_cb * half, cols), low, NT, preferred_element_type=F32)
    rest = rest + lax.dot_general(blocks[:, 1].reshape(n_cb * half, cols), high, NT, preferred_element_type=F32)
    rest = jnp.where(lane == units - first, sums[:, 0].reshape(n_cb * half, 1), rest)
    rest = jnp.where(lane == lanes // 2 + units - first, sums[:, 1].reshape(n_cb * half, 1), rest)
    for j in range(n_cb):
        out[j, :share] = main[j * share : (j + 1) * share]
        out[j, share:] = rest[j * half : (j + 1) * half]


def middle(parts, out):
    n_z0, n_y0, n_cb, held, units = out.shape
    lanes = parts.shape[2]
    share = held * n_z0 * n_y0
    first = lanes - units
    total = parts[0]
    for k in range(1, n_cb):
        total = total + parts[k]
    main, rest = total[:share], total[share:]
    rest = jnp.concatenate([rest[:, : lanes // 2], rest[:, lanes // 2 :]], axis=0)
    inv = lax.rsqrt(rest[:, units - first : units - first + 1] / D + EPS)
    g = main[:, :units] * inv
    u = jnp.concatenate([main[:, units:], rest[:, : units - first]], axis=1) * inv
    hidden = (g / (1.0 + jnp.exp(-g)) * u).astype(BF16).astype(F32)
    r = 4
    n_yq = held // r
    for a in range(n_z0):
        for b in range(n_y0):
            rows = [((a * n_yq + q) * n_y0 + b) * r for q in range(n_yq)]
            block = jnp.concatenate([hidden[s : s + r] for s in rows], axis=0)
            for j in range(n_cb):
                out[a, b, j] = block


def back(here, hid, w0, w1, w2, w3, out):
    acc = None
    for k, w in enumerate((w0, w1, w2, w3)):
        left = hid[here[0] ^ k].astype(BF16)
        part = jnp.dot(left, w[...].astype(BF16), preferred_element_type=F32)
        acc = part if acc is None else acc + part
    n, per, _ = out.shape
    for k in range(n):
        out[k] = acc[k * per : (k + 1) * per]


def fold(here, sums, tok, mixed, sq):
    _, per, _ = sums.shape
    down = jnp.sum(sums[...], axis=0)
    pair = tok[...].astype(F32)
    residual = jnp.where(here[1] % 2 == 1, pair[per:], pair[:per])
    value = 0.1 * residual + down
    mixed[...] = value
    total = jnp.sum(value * value, axis=1, keepdims=True)
    sq[...] = jnp.broadcast_to(total[None], sq.shape)


def finish(mixed, sq, gain, out):
    total = jnp.sum(sq[...], axis=0)[:, :1]
    inv = lax.rsqrt(total / D + EPS)
    out[...] = (mixed[...] * inv * gain[...].astype(F32)).astype(BF16)


def body(tokens, norm_gain, w_gate, w_up, w_down, out_gain):
    n_cb = lax.axis_size("cb")
    n_quad = lax.axis_size(QUAD)
    n_rest = lax.axis_size(REST)
    rows, cols = tokens.shape
    units = w_gate.shape[1]
    own = rows // lax.axis_size(RA)
    share = rows // n_cb
    held = share // n_quad

    mine = w_down.astype(F32)
    others = []
    for k in range(1, n_quad):
        others.append(lax.ppermute(mine, QUAD, [(i, i ^ k) for i in range(n_quad)]))

    lanes = 128
    packed = share + share // 2
    partial = pl.pallas_call(
        front, in_specs=[pl.BlockSpec(memory_space=pltpu.HBM)] * 4,
        out_shape=jax.ShapeDtypeStruct((n_cb, packed, lanes), F32),
        scratch_shapes=[pltpu.VMEM((rows, cols), BF16), pltpu.VMEM((cols,), BF16), pltpu.VMEM((units, cols), BF16),
                        pltpu.VMEM((units, cols), BF16), pltpu.SemaphoreType.DMA((4,))],
        name="front")(tokens, norm_gain, w_gate.T, w_up.T)
    parts = exchange(partial, "cb")
    blocks = pl.pallas_call(middle, out_shape=jax.ShapeDtypeStruct((2, 2, n_cb, held, units), F32), name="middle", compiler_params=SMALL)(parts)
    got = exchange(blocks.reshape(n_quad * n_cb, held, units), QUAD + ("cb",))

    here = jnp.stack([lax.axis_index(QUAD), lax.axis_index(RA)]).astype(jnp.int32)
    sums = pl.pallas_call(
        back,
        grid_spec=pltpu.PrefetchScalarGridSpec(num_scalar_prefetch=1, grid=(1,), in_specs=[
            pl.BlockSpec((n_quad, n_cb * held, units), lambda i, m: (0, 0, 0)),
            *[pl.BlockSpec((units, cols), lambda i, m: (0, 0))] * 4,
        ], out_specs=pl.BlockSpec((n_rest, own, cols), lambda i, m: (0, 0, 0))),
        out_shape=jax.ShapeDtypeStruct((n_rest, own, cols), F32), name="back", compiler_params=SMALL)(
        here, got.reshape(n_quad, n_cb * held, units), w_down, *others)
    sums = exchange(sums, REST)

    mixed, sq = pl.pallas_call(
        fold,
        grid_spec=pltpu.PrefetchScalarGridSpec(num_scalar_prefetch=1, grid=(1,), in_specs=[
            pl.BlockSpec((n_rest, own, cols), lambda i, m: (0, 0, 0)),
            pl.BlockSpec((2 * own, cols), lambda i, m: (m[1] // 2, 0)),
        ], out_specs=[pl.BlockSpec((own, cols), lambda i, m: (0, 0)), pl.BlockSpec((n_cb, own, 128), lambda i, m: (0, 0, 0))]),
        out_shape=[jax.ShapeDtypeStruct((own, cols), F32), jax.ShapeDtypeStruct((n_cb, own, 128), F32)], name="fold", compiler_params=SMALL)(
        here, sums, tokens)
    sq = exchange(sq, "cb")
    return pl.pallas_call(finish, out_shape=jax.ShapeDtypeStruct((own, cols), BF16), name="finish", compiler_params=SMALL)(
        mixed, sq, out_gain[None, :])


def solution(mesh):
    finer = Mesh(mesh.devices.reshape(8, 2, 4, 2, mesh.shape["cb"]), (*RA, "cb"))
    placed = (P(None, "cb"), P("cb"), P("cb", RA), P("cb", RA), P(RA, "cb"), P("cb"))
    return jax.shard_map(body, mesh=finer, in_specs=placed, out_specs=P(RA, "cb"), check_vma=False)
```

```python
import jax
import jax.numpy as jnp
from jax import lax
from jax.experimental import pallas as pl
from jax.experimental.pallas import tpu as pltpu
from jax.sharding import Mesh
from jax.sharding import PartitionSpec as P


D = 4096
EPS = 1e-06
RA = ("zq", "z0", "yq", "y0")
QUAD = ("z0", "y0")
REST = ("zq", "yq")
NT = (((1,), (1,)), ((), ()))
F32 = jnp.float32
BF16 = jnp.bfloat16
SMALL = pltpu.CompilerParams(vmem_limit_bytes=8 * 1024 * 1024)


def exchange(array, axes):
    return lax.all_to_all(array, axes, split_axis=0, concat_axis=0, tiled=True)


def copies(sources, targets, sems):
    started = [pltpu.make_async_copy(s, t, sems.at[k]) for k, (s, t) in enumerate(zip(sources, targets))]
    for c in started:
        c.start()
    return started


def front(tok_hbm, gain_hbm, wg_hbm, wu_hbm, out, tok, gain, wg, wu, sems):
    n_cb, _, lanes = out.shape
    n_chunk, chunk, cols = tok.shape
    units = wg.shape[0]
    share = n_chunk * chunk // n_cb
    half = share // 2
    first = lanes - units
    chunks = [tok_hbm.at[pl.ds(c * chunk, chunk)] for c in range(n_chunk)]
    pending = copies((wg_hbm, wu_hbm, gain_hbm, *chunks), (wg, wu, gain, *[tok.at[c] for c in range(n_chunk)]), sems)
    pending[0].wait()
    pending[1].wait()
    up = wu[...].astype(F32)
    left = jnp.concatenate([wg[...].astype(F32), up[:first]], axis=0).astype(BF16)
    gap = jnp.zeros((lanes // 2 - (units - first), cols), F32)
    none = jnp.zeros((lanes // 2, cols), F32)
    low = jnp.concatenate([up[first:], gap, none], axis=0).astype(BF16)
    high = jnp.concatenate([none, up[first:], gap], axis=0).astype(BF16)
    pending[2].wait()
    scale = gain[...].astype(F32).reshape(1, cols)
    per = chunk // share
    lane = lax.broadcasted_iota(jnp.int32, (per * half, lanes), 1)
    for c in range(n_chunk):
        pending[3 + c].wait()
        x = tok[c].astype(F32)
        sq = jnp.sum(x * x, axis=1, keepdims=True)
        scaled = (x * scale).astype(BF16)
        main = lax.dot_general(scaled, left, NT, preferred_element_type=F32)
        cut = lambda v, h: jnp.concatenate([v[p * share + h * half : p * share + (h + 1) * half] for p in range(per)], axis=0)
        rest = lax.dot_general(cut(scaled, 0), low, NT, preferred_element_type=F32)
        rest = rest + lax.dot_general(cut(scaled, 1), high, NT, preferred_element_type=F32)
        rest = jnp.where(lane == units - first, cut(sq, 0), rest)
        rest = jnp.where(lane == lanes // 2 + units - first, cut(sq, 1), rest)
        for p in range(per):
            out[c * per + p, :share] = main[p * share : (p + 1) * share]
            out[c * per + p, share:] = rest[p * half : (p + 1) * half]


def middle(parts, out):
    n_z0, n_y0, n_cb, held, units = out.shape
    lanes = parts.shape[2]
    share = held * n_z0 * n_y0
    first = lanes - units
    total = parts[0]
    for k in range(1, n_cb):
        total = total + parts[k]
    main, rest = total[:share], total[share:]
    rest = jnp.concatenate([rest[:, : lanes // 2], rest[:, lanes // 2 :]], axis=0)
    inv = lax.rsqrt(rest[:, units - first : units - first + 1] / D + EPS)
    g = main[:, :units] * inv
    u = jnp.concatenate([main[:, units:], rest[:, : units - first]], axis=1) * inv
    hidden = (g / (1.0 + jnp.exp(-g)) * u).astype(BF16).astype(F32)
    r = 4
    n_yq = held // r
    for a in range(n_z0):
        for b in range(n_y0):
            rows = [((a * n_yq + q) * n_y0 + b) * r for q in range(n_yq)]
            block = jnp.concatenate([hidden[s : s + r] for s in rows], axis=0)
            for j in range(n_cb):
                out[a, b, j] = block


def back(here, hid, w0, w1, w2, w3, out):
    acc = None
    for k, w in enumerate((w0, w1, w2, w3)):
        left = hid[here[0] ^ k].astype(BF16)
        part = jnp.dot(left, w[...].astype(BF16), preferred_element_type=F32)
        acc = part if acc is None else acc + part
    n, per, _ = out.shape
    for k in range(n):
        out[k] = acc[k * per : (k + 1) * per]


def fold(sums, residual, gain, gained, sq):
    value = 0.1 * residual[...].astype(F32) + jnp.sum(sums[...], axis=0)
    gained[...] = value * gain[...].astype(F32)
    total = jnp.sum(value * value, axis=1, keepdims=True)
    sq[...] = jnp.broadcast_to(total[None], sq.shape)


def finish(gained, sq, out):
    total = jnp.sum(sq[...], axis=0)[:, :1]
    out[...] = (gained[...] * lax.rsqrt(total / D + EPS)).astype(BF16)


def body(tokens, norm_gain, w_gate, w_up, w_down, out_gain):
    n_cb = lax.axis_size("cb")
    n_quad = lax.axis_size(QUAD)
    n_rest = lax.axis_size(REST)
    rows, cols = tokens.shape
    units = w_gate.shape[1]
    own = rows // lax.axis_size(RA)
    share = rows // n_cb
    held = share // n_quad

    mine = w_down.astype(F32)
    others = []
    for k in range(1, n_quad):
        others.append(lax.ppermute(mine, QUAD, [(i, i ^ k) for i in range(n_quad)]))

    lanes = 128
    packed = share + share // 2
    partial = pl.pallas_call(
        front, in_specs=[pl.BlockSpec(memory_space=pltpu.HBM)] * 4,
        out_shape=jax.ShapeDtypeStruct((n_cb, packed, lanes), F32),
        scratch_shapes=[pltpu.VMEM((4, rows // 4, cols), BF16), pltpu.VMEM((cols,), BF16), pltpu.VMEM((units, cols), BF16),
                        pltpu.VMEM((units, cols), BF16), pltpu.SemaphoreType.DMA((7,))],
        name="front")(tokens, norm_gain, w_gate.T, w_up.T)
    parts = exchange(partial, "cb")
    blocks = pl.pallas_call(middle, out_shape=jax.ShapeDtypeStruct((2, 2, n_cb, held, units), F32), name="middle", compiler_params=SMALL)(parts)
    got = exchange(blocks.reshape(n_quad * n_cb, held, units), QUAD + ("cb",))

    here = lax.axis_index(QUAD).astype(jnp.int32)[None]
    sums = pl.pallas_call(
        back,
        grid_spec=pltpu.PrefetchScalarGridSpec(num_scalar_prefetch=1, grid=(1,), in_specs=[
            pl.BlockSpec((n_quad, n_cb * held, units), lambda i, m: (0, 0, 0)),
            *[pl.BlockSpec((units, cols), lambda i, m: (0, 0))] * 4,
        ], out_specs=pl.BlockSpec((n_rest, own, cols), lambda i, m: (0, 0, 0))),
        out_shape=jax.ShapeDtypeStruct((n_rest, own, cols), F32), name="back", compiler_params=SMALL)(
        here, got.reshape(n_quad, n_cb * held, units), w_down, *others)
    sums = exchange(sums, REST)

    residual = lax.dynamic_slice_in_dim(tokens, lax.axis_index(RA) * own, own, 0)
    gained, sq = pl.pallas_call(
        fold, out_shape=[jax.ShapeDtypeStruct((own, cols), F32), jax.ShapeDtypeStruct((n_cb, own, 128), F32)], name="fold", compiler_params=SMALL)(
        sums, residual, out_gain[None, :])
    sq = exchange(sq, "cb")
    return pl.pallas_call(finish, out_shape=jax.ShapeDtypeStruct((own, cols), BF16), name="finish", compiler_params=SMALL)(gained, sq)


def solution(mesh):
    finer = Mesh(mesh.devices.reshape(8, 2, 4, 2, mesh.shape["cb"]), (*RA, "cb"))
    placed = (P(None, "cb"), P("cb"), P("cb", RA), P("cb", RA), P(RA, "cb"), P("cb"))
    return jax.shard_map(body, mesh=finer, in_specs=placed, out_specs=P(RA, "cb"), check_vma=False)
```

```python
import jax
import jax.numpy as jnp
from jax import lax
from jax.experimental import pallas as pl
from jax.experimental.pallas import tpu as pltpu
from jax.sharding import Mesh
from jax.sharding import PartitionSpec as P


D = 4096
EPS = 1e-06
RA = ("zq", "z0", "yq", "y0")
QUAD = ("z0", "y0")
REST = ("zq", "yq")
NT = (((1,), (1,)), ((), ()))
F32 = jnp.float32
BF16 = jnp.bfloat16
SMALL = pltpu.CompilerParams(vmem_limit_bytes=8 * 1024 * 1024)


def exchange(array, axes):
    return lax.all_to_all(array, axes, split_axis=0, concat_axis=0, tiled=True)


def front(tok, gain, wg, wu, out):
    n_cb, _, lanes = out.shape
    rows, cols = tok.shape
    units = wg.shape[0]
    share = rows // n_cb
    half = share // 2
    first = lanes - units
    x = tok[...].astype(F32)
    sq = jnp.sum(x * x, axis=1, keepdims=True)
    scaled = (x * gain[...].astype(F32).reshape(1, cols)).astype(BF16)
    up = wu[...].astype(F32)
    left = jnp.concatenate([wg[...].astype(F32), up[:first]], axis=0).astype(BF16)
    gap = jnp.zeros((lanes // 2 - (units - first), cols), F32)
    none = jnp.zeros((lanes // 2, cols), F32)
    low = jnp.concatenate([up[first:], gap, none], axis=0).astype(BF16)
    high = jnp.concatenate([none, up[first:], gap], axis=0).astype(BF16)
    main = lax.dot_general(scaled, left, NT, preferred_element_type=F32)
    blocks = scaled.reshape(n_cb, 2, half, cols)
    sums = sq.reshape(n_cb, 2, half, 1)
    lane = lax.broadcasted_iota(jnp.int32, (n_cb * half, lanes), 1)
    rest = lax.dot_general(blocks[:, 0].reshape(n_cb * half, cols), low, NT, preferred_element_type=F32)
    rest = rest + lax.dot_general(blocks[:, 1].reshape(n_cb * half, cols), high, NT, preferred_element_type=F32)
    rest = jnp.where(lane == units - first, sums[:, 0].reshape(n_cb * half, 1), rest)
    rest = jnp.where(lane == lanes // 2 + units - first, sums[:, 1].reshape(n_cb * half, 1), rest)
    for j in range(n_cb):
        out[j, :share] = main[j * share : (j + 1) * share]
        out[j, share:] = rest[j * half : (j + 1) * half]


def middle(parts, out):
    n_z0, n_y0, n_cb, held, units = out.shape
    lanes = parts.shape[2]
    share = held * n_z0 * n_y0
    first = lanes - units
    total = parts[0]
    for k in range(1, n_cb):
        total = total + parts[k]
    main, rest = total[:share], total[share:]
    rest = jnp.concatenate([rest[:, : lanes // 2], rest[:, lanes // 2 :]], axis=0)
    inv = lax.rsqrt(rest[:, units - first : units - first + 1] / D + EPS)
    g = main[:, :units] * inv
    u = jnp.concatenate([main[:, units:], rest[:, : units - first]], axis=1) * inv
    hidden = (g / (1.0 + jnp.exp(-g)) * u).astype(BF16).astype(F32)
    r = 4
    n_yq = held // r
    for a in range(n_z0):
        for b in range(n_y0):
            rows = [((a * n_yq + q) * n_y0 + b) * r for q in range(n_yq)]
            block = jnp.concatenate([hidden[s : s + r] for s in rows], axis=0)
            for j in range(n_cb):
                out[a, b, j] = block


def back(here, hid, w0, w1, w2, w3, _residual, _gain, out):
    acc = None
    for k, w in enumerate((w0, w1, w2, w3)):
        left = hid[here[0] ^ k].astype(BF16)
        part = jnp.dot(left, w[...].astype(BF16), preferred_element_type=F32)
        acc = part if acc is None else acc + part
    n, per, _ = out.shape
    for k in range(n):
        out[k] = acc[k * per : (k + 1) * per]


def fold(sums, residual, gain, gained, sq):
    value = 0.1 * residual[...].astype(F32) + jnp.sum(sums[...], axis=0)
    gained[...] = value * gain[...].astype(F32)
    total = jnp.sum(value * value, axis=1, keepdims=True)
    sq[...] = jnp.broadcast_to(total[None], sq.shape)


def finish(gained, sq, out):
    total = jnp.sum(sq[...], axis=0)[:, :1]
    out[...] = (gained[...] * lax.rsqrt(total / D + EPS)).astype(BF16)


def body(tokens, norm_gain, w_gate, w_up, w_down, out_gain):
    n_cb = lax.axis_size("cb")
    n_quad = lax.axis_size(QUAD)
    n_rest = lax.axis_size(REST)
    rows, cols = tokens.shape
    units = w_gate.shape[1]
    own = rows // lax.axis_size(RA)
    share = rows // n_cb
    held = share // n_quad

    mine = w_down.astype(F32)
    others = []
    for k in range(1, n_quad):
        others.append(lax.ppermute(mine, QUAD, [(i, i ^ k) for i in range(n_quad)]))

    lanes = 128
    packed = share + share // 2
    partial = pl.pallas_call(front, out_shape=jax.ShapeDtypeStruct((n_cb, packed, lanes), F32), name="front", compiler_params=SMALL)(
        tokens, norm_gain, w_gate.T, w_up.T)
    parts = exchange(partial, "cb")
    blocks = pl.pallas_call(middle, out_shape=jax.ShapeDtypeStruct((2, 2, n_cb, held, units), F32), name="middle", compiler_params=SMALL)(parts)
    got = exchange(blocks.reshape(n_quad * n_cb, held, units), QUAD + ("cb",))

    residual = lax.dynamic_slice_in_dim(tokens, lax.axis_index(RA) * own, own, 0)
    wide_gain = out_gain.astype(F32)[None, :]
    here = lax.axis_index(QUAD).astype(jnp.int32)[None]
    sums = pl.pallas_call(
        back,
        grid_spec=pltpu.PrefetchScalarGridSpec(num_scalar_prefetch=1, grid=(1,), in_specs=[
            pl.BlockSpec((n_quad, n_cb * held, units), lambda i, m: (0, 0, 0)),
            *[pl.BlockSpec((units, cols), lambda i, m: (0, 0))] * 4,
            *[pl.BlockSpec(memory_space=pl.ANY)] * 2,
        ], out_specs=pl.BlockSpec((n_rest, own, cols), lambda i, m: (0, 0, 0))),
        out_shape=jax.ShapeDtypeStruct((n_rest, own, cols), F32), name="back", compiler_params=SMALL)(
        here, got.reshape(n_quad, n_cb * held, units), w_down, *others, residual, wide_gain)
    sums = exchange(sums, REST)

    gained, sq = pl.pallas_call(
        fold, out_shape=[jax.ShapeDtypeStruct((own, cols), F32), jax.ShapeDtypeStruct((n_cb, own, 128), F32)], name="fold", compiler_params=SMALL)(
        sums, residual, wide_gain)
    sq = exchange(sq, "cb")
    return pl.pallas_call(finish, out_shape=jax.ShapeDtypeStruct((own, cols), BF16), name="finish", compiler_params=SMALL)(gained, sq)


def solution(mesh):
    finer = Mesh(mesh.devices.reshape(8, 2, 4, 2, mesh.shape["cb"]), (*RA, "cb"))
    placed = (P(None, "cb"), P("cb"), P("cb", RA), P("cb", RA), P(RA, "cb"), P("cb"))
    return jax.shard_map(body, mesh=finer, in_specs=placed, out_specs=P(RA, "cb"), check_vma=False)
```

```python
import jax
import jax.numpy as jnp
from jax import lax
from jax.experimental import pallas as pl
from jax.experimental.pallas import tpu as pltpu
from jax.sharding import Mesh
from jax.sharding import PartitionSpec as P


D = 4096
EPS = 1e-06
RA = ("zq", "z0", "yq", "y0")
QUAD = ("z0", "y0")
REST = ("zq", "yq")
NT = (((1,), (1,)), ((), ()))
F32 = jnp.float32
BF16 = jnp.bfloat16
SMALL = pltpu.CompilerParams(vmem_limit_bytes=8 * 1024 * 1024)


def exchange(array, axes):
    return lax.all_to_all(array, axes, split_axis=0, concat_axis=0, tiled=True)


def enter(here, down_hbm, tok_hbm, gain_hbm, wg_hbm, wu_hbm, last_hbm, wide, last, own, out, narrow, tok, gain, wg, wu, sems):
    rows = own.shape[0]
    source = tok_hbm.at[pl.ds(pl.multiple_of(here[0] // 2 * rows, rows), rows)]
    pairs = ((down_hbm, narrow), (wg_hbm, wg), (wu_hbm, wu), (gain_hbm, gain), (tok_hbm, tok), (last_hbm, last), (source, own))
    pending = [pltpu.make_async_copy(a, b, sems.at[k]) for k, (a, b) in enumerate(pairs)]
    for c in pending:
        c.start()
    pending[0].wait()
    wide[...] = narrow[...].astype(F32)
    for c in pending[1:]:
        c.wait()
    front(tok, gain, wg, wu, out)


def order(here, hid, out):
    quad = here[0] // 8 % 2 * 2 + here[0] % 2
    for k in range(out.shape[0]):
        out[k] = hid[quad ^ k].astype(BF16)


def front(tok, gain, wg, wu, out):
    n_cb, _, lanes = out.shape
    rows, cols = tok.shape
    units = wg.shape[0]
    share = rows // n_cb
    half = share // 2
    first = lanes - units
    x = tok[...].astype(F32)
    sq = jnp.sum(x * x, axis=1, keepdims=True)
    scaled = (x * gain[...].astype(F32).reshape(1, cols)).astype(BF16)
    up = wu[...].astype(F32)
    left = jnp.concatenate([wg[...].astype(F32), up[:first]], axis=0).astype(BF16)
    gap = jnp.zeros((lanes // 2 - (units - first), cols), F32)
    none = jnp.zeros((lanes // 2, cols), F32)
    low = jnp.concatenate([up[first:], gap, none], axis=0).astype(BF16)
    high = jnp.concatenate([none, up[first:], gap], axis=0).astype(BF16)
    main = lax.dot_general(scaled, left, NT, preferred_element_type=F32)
    blocks = scaled.reshape(n_cb, 2, half, cols)
    sums = sq.reshape(n_cb, 2, half, 1)
    lane = lax.broadcasted_iota(jnp.int32, (n_cb * half, lanes), 1)
    rest = lax.dot_general(blocks[:, 0].reshape(n_cb * half, cols), low, NT, preferred_element_type=F32)
    rest = rest + lax.dot_general(blocks[:, 1].reshape(n_cb * half, cols), high, NT, preferred_element_type=F32)
    rest = jnp.where(lane == units - first, sums[:, 0].reshape(n_cb * half, 1), rest)
    rest = jnp.where(lane == lanes // 2 + units - first, sums[:, 1].reshape(n_cb * half, 1), rest)
    for j in range(n_cb):
        out[j, :share] = main[j * share : (j + 1) * share]
        out[j, share:] = rest[j * half : (j + 1) * half]


def middle(parts, out):
    n_z0, n_y0, n_cb, held, units = out.shape
    lanes = parts.shape[2]
    share = held * n_z0 * n_y0
    first = lanes - units
    total = parts[0]
    for k in range(1, n_cb):
        total = total + parts[k]
    main, rest = total[:share], total[share:]
    rest = jnp.concatenate([rest[:, : lanes // 2], rest[:, lanes // 2 :]], axis=0)
    inv = lax.rsqrt(rest[:, units - first : units - first + 1] / D + EPS)
    g = main[:, :units] * inv
    u = jnp.concatenate([main[:, units:], rest[:, : units - first]], axis=1) * inv
    hidden = (g / (1.0 + jnp.exp(-g)) * u).astype(BF16).astype(F32)
    r = 4
    n_yq = held // r
    for a in range(n_z0):
        for b in range(n_y0):
            rows = [((a * n_yq + q) * n_y0 + b) * r for q in range(n_yq)]
            block = jnp.concatenate([hidden[s : s + r] for s in rows], axis=0)
            for j in range(n_cb):
                out[a, b, j] = block


def back(hid, w0, w1, w2, w3, out):
    acc = None
    for k, w in enumerate((w0, w1, w2, w3)):
        part = jnp.dot(hid[k], w[...].astype(BF16), preferred_element_type=F32)
        acc = part if acc is None else acc + part
    n, per, _ = out.shape
    for k in range(n):
        out[k] = acc[k * per : (k + 1) * per]


def fold(here, sums, residual, gain, gained, sq):
    per, cols = gained.shape
    pair = residual[...].astype(F32)
    value = 0.1 * jnp.where(here[0] % 2 == 1, pair[per:], pair[:per]) + jnp.sum(sums[...], axis=0)
    gained[...] = value * gain[...].astype(F32).reshape(1, cols)
    total = jnp.sum(value * value, axis=1, keepdims=True)
    sq[...] = jnp.broadcast_to(total[None], sq.shape)


def finish(gained, sq, out):
    total = jnp.sum(sq[...], axis=0)[:, :1]
    out[...] = (gained[...] * lax.rsqrt(total / D + EPS)).astype(BF16)


def body(tokens, norm_gain, w_gate, w_up, w_down, out_gain):
    n_cb = lax.axis_size("cb")
    n_quad = lax.axis_size(QUAD)
    n_rest = lax.axis_size(REST)
    rows, cols = tokens.shape
    units = w_gate.shape[1]
    own = rows // lax.axis_size(RA)
    share = rows // n_cb
    held = share // n_quad

    here = lax.axis_index(RA).astype(jnp.int32)[None]
    lanes = 128
    packed = share + share // 2
    inputs = (w_down, tokens, norm_gain, w_gate.T, w_up.T, out_gain)
    hbm = [pltpu.with_memory_space_constraint(x, pltpu.HBM) for x in inputs]
    whole = lambda *shape: pl.BlockSpec(shape, lambda i, m: (0,) * len(shape))
    mine, out_gain, residual, partial = pl.pallas_call(
        enter,
        grid_spec=pltpu.PrefetchScalarGridSpec(
            num_scalar_prefetch=1, grid=(1,), in_specs=[pl.BlockSpec(memory_space=pltpu.HBM)] * 6,
            out_specs=[whole(units, cols), whole(cols), whole(2 * own, cols), whole(n_cb, packed, lanes)],
            scratch_shapes=[pltpu.VMEM((units, cols), BF16), pltpu.VMEM((rows, cols), BF16), pltpu.VMEM((cols,), BF16),
                            pltpu.VMEM((units, cols), BF16), pltpu.VMEM((units, cols), BF16), pltpu.SemaphoreType.DMA((7,))]),
        out_shape=[jax.ShapeDtypeStruct((units, cols), F32), jax.ShapeDtypeStruct((cols,), BF16), jax.ShapeDtypeStruct((2 * own, cols), BF16),
                   jax.ShapeDtypeStruct((n_cb, packed, lanes), F32)],
        name="enter", compiler_params=SMALL)(here, *hbm)
    others = []
    for k in range(1, n_quad):
        others.append(lax.ppermute(mine, QUAD, [(i, i ^ k) for i in range(n_quad)]))

    parts = exchange(partial, "cb")
    blocks = pl.pallas_call(middle, out_shape=jax.ShapeDtypeStruct((2, 2, n_cb, held, units), F32), name="middle", compiler_params=SMALL)(parts)
    got = exchange(blocks.reshape(n_quad * n_cb, held, units), QUAD + ("cb",))

    hidden = pl.pallas_call(
        order,
        grid_spec=pltpu.PrefetchScalarGridSpec(
            num_scalar_prefetch=1, grid=(1,), in_specs=[pl.BlockSpec((n_quad, n_cb * held, units), lambda i, m: (0, 0, 0))],
            out_specs=pl.BlockSpec((n_quad, n_cb * held, units), lambda i, m: (0, 0, 0))),
        out_shape=jax.ShapeDtypeStruct((n_quad, n_cb * held, units), BF16), name="order", compiler_params=SMALL)(
        here, got.reshape(n_quad, n_cb * held, units))
    sums = pl.pallas_call(back, out_shape=jax.ShapeDtypeStruct((n_rest, own, cols), F32), name="back", compiler_params=SMALL)(
        hidden, mine, *others)
    sums = exchange(sums, REST)

    gained, sq = pl.pallas_call(
        fold,
        grid_spec=pltpu.PrefetchScalarGridSpec(
            num_scalar_prefetch=1, grid=(1,), in_specs=[
                pl.BlockSpec((n_rest, own, cols), lambda i, m: (0, 0, 0)), pl.BlockSpec((2 * own, cols), lambda i, m: (0, 0)),
                pl.BlockSpec((cols,), lambda i, m: (0,))],
            out_specs=[pl.BlockSpec((own, cols), lambda i, m: (0, 0)), pl.BlockSpec((n_cb, own, 128), lambda i, m: (0, 0, 0))]),
        out_shape=[jax.ShapeDtypeStruct((own, cols), F32), jax.ShapeDtypeStruct((n_cb, own, 128), F32)], name="fold", compiler_params=SMALL)(
        here, sums, residual, out_gain)
    sq = exchange(sq, "cb")
    return pl.pallas_call(finish, out_shape=jax.ShapeDtypeStruct((own, cols), BF16), name="finish", compiler_params=SMALL)(gained, sq)


def solution(mesh):
    finer = Mesh(mesh.devices.reshape(8, 2, 4, 2, mesh.shape["cb"]), (*RA, "cb"))
    placed = (P(None, "cb"), P("cb"), P("cb", RA), P("cb", RA), P(RA, "cb"), P("cb"))
    return jax.shard_map(body, mesh=finer, in_specs=placed, out_specs=P(RA, "cb"), check_vma=False)
```

```python
import jax
import jax.numpy as jnp
from jax import lax
from jax.experimental import pallas as pl
from jax.experimental.pallas import tpu as pltpu
from jax.sharding import Mesh
from jax.sharding import PartitionSpec as P


D = 4096
EPS = 1e-06
RA = ("zq", "z0", "yq", "y0")
QUAD = ("z0", "y0")
REST = ("zq", "yq")
NT = (((1,), (1,)), ((), ()))
F32 = jnp.float32
BF16 = jnp.bfloat16
SMALL = pltpu.CompilerParams(vmem_limit_bytes=8 * 1024 * 1024)


def exchange(array, axes):
    return lax.all_to_all(array, axes, split_axis=0, concat_axis=0, tiled=True)


def enter(here, down_hbm, tok_hbm, gain_hbm, wg_hbm, wu_hbm, last_hbm, wide, last, own, out, narrow, tok, gain, wg, wu, sems):
    rows = own.shape[0]
    source = tok_hbm.at[pl.ds(pl.multiple_of(here[0] // 2 * rows, rows), rows)]
    pairs = ((down_hbm, narrow), (wg_hbm, wg), (wu_hbm, wu), (gain_hbm, gain), (tok_hbm, tok), (last_hbm, last), (source, own))
    pending = [pltpu.make_async_copy(a, b, sems.at[k]) for k, (a, b) in enumerate(pairs)]
    for c in pending:
        c.start()
    pending[0].wait()
    wide[...] = narrow[...].astype(F32)
    for c in pending[1:]:
        c.wait()
    front(tok, gain, wg, wu, out)


def order(here, hid, out):
    quad = here[0] // 8 % 2 * 2 + here[0] % 2
    for k in range(out.shape[0]):
        for j in range(hid.shape[0]):
            held = hid.shape[2]
            out[k, j * held : (j + 1) * held] = hid[j, quad ^ k].astype(BF16)


def front(tok, gain, wg, wu, out):
    n_cb, _, lanes = out.shape
    rows, cols = tok.shape
    units = wg.shape[0]
    share = rows // n_cb
    half = share // 2
    first = lanes - units
    x = tok[...].astype(F32)
    sq = jnp.sum(x * x, axis=1, keepdims=True)
    scaled = (x * gain[...].astype(F32).reshape(1, cols)).astype(BF16)
    up = wu[...].astype(F32)
    left = jnp.concatenate([wg[...].astype(F32), up[:first]], axis=0).astype(BF16)
    gap = jnp.zeros((lanes // 2 - (units - first), cols), F32)
    none = jnp.zeros((lanes // 2, cols), F32)
    low = jnp.concatenate([up[first:], gap, none], axis=0).astype(BF16)
    high = jnp.concatenate([none, up[first:], gap], axis=0).astype(BF16)
    main = lax.dot_general(scaled, left, NT, preferred_element_type=F32)
    blocks = scaled.reshape(n_cb, 2, half, cols)
    sums = sq.reshape(n_cb, 2, half, 1)
    lane = lax.broadcasted_iota(jnp.int32, (n_cb * half, lanes), 1)
    rest = lax.dot_general(blocks[:, 0].reshape(n_cb * half, cols), low, NT, preferred_element_type=F32)
    rest = rest + lax.dot_general(blocks[:, 1].reshape(n_cb * half, cols), high, NT, preferred_element_type=F32)
    rest = jnp.where(lane == units - first, sums[:, 0].reshape(n_cb * half, 1), rest)
    rest = jnp.where(lane == lanes // 2 + units - first, sums[:, 1].reshape(n_cb * half, 1), rest)
    for j in range(n_cb):
        out[j, :share] = main[j * share : (j + 1) * share]
        out[j, share:] = rest[j * half : (j + 1) * half]


def middle(parts, out):
    n_cb, n_z0, n_y0, held, units = out.shape
    lanes = parts.shape[2]
    share = held * n_z0 * n_y0
    first = lanes - units
    total = parts[0]
    for k in range(1, n_cb):
        total = total + parts[k]
    main, rest = total[:share], total[share:]
    rest = jnp.concatenate([rest[:, : lanes // 2], rest[:, lanes // 2 :]], axis=0)
    inv = lax.rsqrt(rest[:, units - first : units - first + 1] / D + EPS)
    g = main[:, :units] * inv
    u = jnp.concatenate([main[:, units:], rest[:, : units - first]], axis=1) * inv
    hidden = (g / (1.0 + jnp.exp(-g)) * u).astype(BF16).astype(F32)
    r = 4
    n_yq = held // r
    for a in range(n_z0):
        for b in range(n_y0):
            rows = [((a * n_yq + q) * n_y0 + b) * r for q in range(n_yq)]
            block = jnp.concatenate([hidden[s : s + r] for s in rows], axis=0)
            for j in range(n_cb):
                out[j, a, b] = block


def back(hid, w0, w1, w2, w3, out):
    acc = None
    for k, w in enumerate((w0, w1, w2, w3)):
        part = jnp.dot(hid[k], w[...].astype(BF16), preferred_element_type=F32)
        acc = part if acc is None else acc + part
    n, per, _ = out.shape
    for k in range(n):
        out[k] = acc[k * per : (k + 1) * per]


def fold(here, sums, residual, gain, gained, sq):
    per, cols = gained.shape
    pair = residual[...].astype(F32)
    value = 0.1 * jnp.where(here[0] % 2 == 1, pair[per:], pair[:per]) + jnp.sum(sums[...], axis=0)
    gained[...] = value * gain[...].astype(F32).reshape(1, cols)
    total = jnp.sum(value * value, axis=1, keepdims=True)
    sq[...] = jnp.broadcast_to(total[None], sq.shape)


def finish(gained, sq, out):
    total = jnp.sum(sq[...], axis=0)[:, :1]
    out[...] = (gained[...] * lax.rsqrt(total / D + EPS)).astype(BF16)


def body(tokens, norm_gain, w_gate, w_up, w_down, out_gain):
    n_cb = lax.axis_size("cb")
    n_quad = lax.axis_size(QUAD)
    n_rest = lax.axis_size(REST)
    rows, cols = tokens.shape
    units = w_gate.shape[1]
    own = rows // lax.axis_size(RA)
    share = rows // n_cb
    held = share // n_quad

    here = lax.axis_index(RA).astype(jnp.int32)[None]
    lanes = 128
    packed = share + share // 2
    inputs = (w_down, tokens, norm_gain, w_gate.T, w_up.T, out_gain)
    hbm = [pltpu.with_memory_space_constraint(x, pltpu.HBM) for x in inputs]
    whole = lambda *shape: pl.BlockSpec(shape, lambda i, m: (0,) * len(shape))
    mine, out_gain, residual, partial = pl.pallas_call(
        enter,
        grid_spec=pltpu.PrefetchScalarGridSpec(
            num_scalar_prefetch=1, grid=(1,), in_specs=[pl.BlockSpec(memory_space=pltpu.HBM)] * 6,
            out_specs=[whole(units, cols), whole(cols), whole(2 * own, cols), whole(n_cb, packed, lanes)],
            scratch_shapes=[pltpu.VMEM((units, cols), BF16), pltpu.VMEM((rows, cols), BF16), pltpu.VMEM((cols,), BF16),
                            pltpu.VMEM((units, cols), BF16), pltpu.VMEM((units, cols), BF16), pltpu.SemaphoreType.DMA((7,))]),
        out_shape=[jax.ShapeDtypeStruct((units, cols), F32), jax.ShapeDtypeStruct((cols,), BF16), jax.ShapeDtypeStruct((2 * own, cols), BF16),
                   jax.ShapeDtypeStruct((n_cb, packed, lanes), F32)],
        name="enter", compiler_params=SMALL)(here, *hbm)
    others = []
    for k in range(1, n_quad):
        others.append(lax.ppermute(mine, QUAD, [(i, i ^ k) for i in range(n_quad)]))

    parts = exchange(partial, "cb")
    blocks = pl.pallas_call(middle, out_shape=jax.ShapeDtypeStruct((n_cb, 2, 2, held, units), F32), name="middle", compiler_params=SMALL)(parts)
    got = exchange(blocks.reshape(n_quad * n_cb, held, units), ("cb",) + QUAD)

    hidden = pl.pallas_call(
        order,
        grid_spec=pltpu.PrefetchScalarGridSpec(
            num_scalar_prefetch=1, grid=(1,), in_specs=[pl.BlockSpec((n_cb, n_quad, held, units), lambda i, m: (0, 0, 0, 0))],
            out_specs=pl.BlockSpec((n_quad, n_cb * held, units), lambda i, m: (0, 0, 0))),
        out_shape=jax.ShapeDtypeStruct((n_quad, n_cb * held, units), BF16), name="order", compiler_params=SMALL)(
        here, got.reshape(n_cb, n_quad, held, units))
    sums = pl.pallas_call(back, out_shape=jax.ShapeDtypeStruct((n_rest, own, cols), F32), name="back", compiler_params=SMALL)(
        hidden, mine, *others)
    sums = exchange(sums, REST)

    gained, sq = pl.pallas_call(
        fold,
        grid_spec=pltpu.PrefetchScalarGridSpec(
            num_scalar_prefetch=1, grid=(1,), in_specs=[
                pl.BlockSpec((n_rest, own, cols), lambda i, m: (0, 0, 0)), pl.BlockSpec((2 * own, cols), lambda i, m: (0, 0)),
                pl.BlockSpec((cols,), lambda i, m: (0,))],
            out_specs=[pl.BlockSpec((own, cols), lambda i, m: (0, 0)), pl.BlockSpec((n_cb, own, 128), lambda i, m: (0, 0, 0))]),
        out_shape=[jax.ShapeDtypeStruct((own, cols), F32), jax.ShapeDtypeStruct((n_cb, own, 128), F32)], name="fold", compiler_params=SMALL)(
        here, sums, residual, out_gain)
    sq = exchange(sq, "cb")
    return pl.pallas_call(finish, out_shape=jax.ShapeDtypeStruct((own, cols), BF16), name="finish", compiler_params=SMALL)(gained, sq)


def solution(mesh):
    finer = Mesh(mesh.devices.reshape(8, 2, 4, 2, mesh.shape["cb"]), (*RA, "cb"))
    placed = (P(None, "cb"), P("cb"), P("cb", RA), P("cb", RA), P(RA, "cb"), P("cb"))
    return jax.shard_map(body, mesh=finer, in_specs=placed, out_specs=P(RA, "cb"), check_vma=False)
```

```python
import jax
import jax.numpy as jnp
from jax import lax
from jax.experimental import pallas as pl
from jax.experimental.pallas import tpu as pltpu
from jax.sharding import Mesh
from jax.sharding import PartitionSpec as P


D = 4096
EPS = 1e-06
RA = ("zq", "z0", "yq", "y0")
QUAD = ("z0", "y0")
REST = ("zq", "yq")
NT = (((1,), (1,)), ((), ()))
F32 = jnp.float32
BF16 = jnp.bfloat16
SMALL = pltpu.CompilerParams(vmem_limit_bytes=8 * 1024 * 1024)


def exchange(array, axes):
    return lax.all_to_all(array, axes, split_axis=0, concat_axis=0, tiled=True)


def enter(here, down_hbm, tok_hbm, gain_hbm, wg_hbm, wu_hbm, last_hbm, wide, last, own, out, narrow, tok, gain, wg, wu, sems):
    rows = own.shape[0]
    source = tok_hbm.at[pl.ds(pl.multiple_of(here[0] // 2 * rows, rows), rows)]
    pairs = ((down_hbm, narrow), (wg_hbm, wg), (wu_hbm, wu), (gain_hbm, gain), (tok_hbm, tok), (last_hbm, last), (source, own))
    pending = [pltpu.make_async_copy(a, b, sems.at[k]) for k, (a, b) in enumerate(pairs)]
    for c in pending:
        c.start()
    pending[0].wait()
    wide[...] = narrow[...].astype(F32)
    for c in pending[1:]:
        c.wait()
    front(tok, gain, wg, wu, out)


def order(here, hid, out):
    quad = here[0] // 8 % 2 * 2 + here[0] % 2
    for k in range(out.shape[0]):
        for j in range(hid.shape[0]):
            held = hid.shape[2]
            out[k, j * held : (j + 1) * held] = hid[j, quad ^ k].astype(BF16)


def front(tok, gain, wg, wu, out):
    n_cb, _, lanes = out.shape
    rows, cols = tok.shape
    units = wg.shape[0]
    share = rows // n_cb
    half = share // 2
    first = lanes - units
    x = tok[...].astype(F32)
    sq = jnp.sum(x * x, axis=1, keepdims=True)
    scaled = (x * gain[...].astype(F32).reshape(1, cols)).astype(BF16)
    up = wu[...].astype(F32)
    left = jnp.concatenate([wg[...].astype(F32), up[:first]], axis=0).astype(BF16)
    gap = jnp.zeros((lanes // 2 - (units - first), cols), F32)
    none = jnp.zeros((lanes // 2, cols), F32)
    low = jnp.concatenate([up[first:], gap, none], axis=0).astype(BF16)
    high = jnp.concatenate([none, up[first:], gap], axis=0).astype(BF16)
    main = lax.dot_general(scaled, left, NT, preferred_element_type=F32)
    blocks = scaled.reshape(n_cb, 2, half, cols)
    sums = sq.reshape(n_cb, 2, half, 1)
    lane = lax.broadcasted_iota(jnp.int32, (n_cb * half, lanes), 1)
    rest = lax.dot_general(blocks[:, 0].reshape(n_cb * half, cols), low, NT, preferred_element_type=F32)
    rest = rest + lax.dot_general(blocks[:, 1].reshape(n_cb * half, cols), high, NT, preferred_element_type=F32)
    rest = jnp.where(lane == units - first, sums[:, 0].reshape(n_cb * half, 1), rest)
    rest = jnp.where(lane == lanes // 2 + units - first, sums[:, 1].reshape(n_cb * half, 1), rest)
    for j in range(n_cb):
        out[j, :share] = main[j * share : (j + 1) * share]
        out[j, share:] = rest[j * half : (j + 1) * half]


def middle(parts, out):
    n_cb, n_z0, n_y0, held, units = out.shape
    lanes = parts.shape[2]
    share = held * n_z0 * n_y0
    first = lanes - units
    total = parts[0]
    for k in range(1, n_cb):
        total = total + parts[k]
    main, rest = total[:share], total[share:]
    rest = jnp.concatenate([rest[:, : lanes // 2], rest[:, lanes // 2 :]], axis=0)
    inv = lax.rsqrt(rest[:, units - first : units - first + 1] / D + EPS)
    g = main[:, :units] * inv
    u = jnp.concatenate([main[:, units:], rest[:, : units - first]], axis=1) * inv
    hidden = (g / (1.0 + jnp.exp(-g)) * u).astype(BF16).astype(F32)
    r = 4
    n_yq = held // r
    for a in range(n_z0):
        for b in range(n_y0):
            rows = [((a * n_yq + q) * n_y0 + b) * r for q in range(n_yq)]
            block = jnp.concatenate([hidden[s : s + r] for s in rows], axis=0)
            for j in range(n_cb):
                out[j, a, b] = block


def back(hid, w0, w1, w2, w3, out):
    acc = None
    for k, w in enumerate((w0, w1, w2, w3)):
        part = jnp.dot(hid[k], w[...].astype(BF16), preferred_element_type=F32)
        acc = part if acc is None else acc + part
    n, held, lanes = out.shape
    blocks = acc.shape[1] // lanes
    per = held // blocks
    for k in range(n):
        out[k] = jnp.concatenate([acc[k * per : (k + 1) * per, b * lanes : (b + 1) * lanes] for b in range(blocks)], axis=0)


def fold(here, sums, residual, gain, gained, sq):
    per, cols = gained.shape
    pair = residual[...].astype(F32)
    down = jnp.sum(sums[...], axis=0)
    down = jnp.concatenate([down[b * per : (b + 1) * per] for b in range(down.shape[0] // per)], axis=1)
    value = 0.1 * jnp.where(here[0] % 2 == 1, pair[per:], pair[:per]) + down
    gained[...] = value * gain[...].astype(F32).reshape(1, cols)
    total = jnp.sum(value * value, axis=1, keepdims=True)
    sq[...] = jnp.broadcast_to(total[None], sq.shape)


def finish(gained, sq, out):
    total = jnp.sum(sq[...], axis=0)[:, :1]
    out[...] = (gained[...] * lax.rsqrt(total / D + EPS)).astype(BF16)


def body(tokens, norm_gain, w_gate, w_up, w_down, out_gain):
    n_cb = lax.axis_size("cb")
    n_quad = lax.axis_size(QUAD)
    n_rest = lax.axis_size(REST)
    rows, cols = tokens.shape
    units = w_gate.shape[1]
    own = rows // lax.axis_size(RA)
    share = rows // n_cb
    held = share // n_quad

    here = lax.axis_index(RA).astype(jnp.int32)[None]
    lanes = 128
    packed = share + share // 2
    inputs = (w_down, tokens, norm_gain, w_gate.T, w_up.T, out_gain)
    hbm = [pltpu.with_memory_space_constraint(x, pltpu.HBM) for x in inputs]
    whole = lambda *shape: pl.BlockSpec(shape, lambda i, m: (0,) * len(shape))
    mine, out_gain, residual, partial = pl.pallas_call(
        enter,
        grid_spec=pltpu.PrefetchScalarGridSpec(
            num_scalar_prefetch=1, grid=(1,), in_specs=[pl.BlockSpec(memory_space=pltpu.HBM)] * 6,
            out_specs=[whole(units, cols), whole(cols), whole(2 * own, cols), whole(n_cb, packed, lanes)],
            scratch_shapes=[pltpu.VMEM((units, cols), BF16), pltpu.VMEM((rows, cols), BF16), pltpu.VMEM((cols,), BF16),
                            pltpu.VMEM((units, cols), BF16), pltpu.VMEM((units, cols), BF16), pltpu.SemaphoreType.DMA((7,))]),
        out_shape=[jax.ShapeDtypeStruct((units, cols), F32), jax.ShapeDtypeStruct((cols,), BF16), jax.ShapeDtypeStruct((2 * own, cols), BF16),
                   jax.ShapeDtypeStruct((n_cb, packed, lanes), F32)],
        name="enter", compiler_params=SMALL)(here, *hbm)
    others = []
    for k in range(1, n_quad):
        others.append(lax.ppermute(mine, QUAD, [(i, i ^ k) for i in range(n_quad)]))

    parts = exchange(partial, "cb")
    blocks = pl.pallas_call(middle, out_shape=jax.ShapeDtypeStruct((n_cb, 2, 2, held, units), F32), name="middle", compiler_params=SMALL)(parts)
    got = exchange(blocks.reshape(n_quad * n_cb, held, units), ("cb",) + QUAD)

    hidden = pl.pallas_call(
        order,
        grid_spec=pltpu.PrefetchScalarGridSpec(
            num_scalar_prefetch=1, grid=(1,), in_specs=[pl.BlockSpec((n_cb, n_quad, held, units), lambda i, m: (0, 0, 0, 0))],
            out_specs=pl.BlockSpec((n_quad, n_cb * held, units), lambda i, m: (0, 0, 0))),
        out_shape=jax.ShapeDtypeStruct((n_quad, n_cb * held, units), BF16), name="order", compiler_params=SMALL)(
        here, got.reshape(n_cb, n_quad, held, units))
    sums = pl.pallas_call(back, out_shape=jax.ShapeDtypeStruct((n_rest, own * cols // 128, 128), F32), name="back", compiler_params=SMALL)(
        hidden, mine, *others)
    sums = exchange(sums, REST)

    gained, sq = pl.pallas_call(
        fold,
        grid_spec=pltpu.PrefetchScalarGridSpec(
            num_scalar_prefetch=1, grid=(1,), in_specs=[
                pl.BlockSpec((n_rest, own * cols // 128, 128), lambda i, m: (0, 0, 0)), pl.BlockSpec((2 * own, cols), lambda i, m: (0, 0)),
                pl.BlockSpec((cols,), lambda i, m: (0,))],
            out_specs=[pl.BlockSpec((own, cols), lambda i, m: (0, 0)), pl.BlockSpec((n_cb, own, 128), lambda i, m: (0, 0, 0))]),
        out_shape=[jax.ShapeDtypeStruct((own, cols), F32), jax.ShapeDtypeStruct((n_cb, own, 128), F32)], name="fold", compiler_params=SMALL)(
        here, sums, residual, out_gain)
    sq = exchange(sq, "cb")
    return pl.pallas_call(finish, out_shape=jax.ShapeDtypeStruct((own, cols), BF16), name="finish", compiler_params=SMALL)(gained, sq)


def solution(mesh):
    finer = Mesh(mesh.devices.reshape(8, 2, 4, 2, mesh.shape["cb"]), (*RA, "cb"))
    placed = (P(None, "cb"), P("cb"), P("cb", RA), P("cb", RA), P(RA, "cb"), P("cb"))
    return jax.shard_map(body, mesh=finer, in_specs=placed, out_specs=P(RA, "cb"), check_vma=False)
```

```python
import jax
import jax.numpy as jnp
from jax import lax
from jax.experimental import pallas as pl
from jax.experimental.pallas import tpu as pltpu
from jax.sharding import Mesh
from jax.sharding import PartitionSpec as P


D = 4096
EPS = 1e-06
RA = ("zq", "z0", "yq", "y0")
QUAD = ("z0", "y0")
REST = ("zq", "yq")
NT = (((1,), (1,)), ((), ()))
F32 = jnp.float32
BF16 = jnp.bfloat16
SMALL = pltpu.CompilerParams(vmem_limit_bytes=8 * 1024 * 1024)


def exchange(array, axes):
    return lax.all_to_all(array, axes, split_axis=0, concat_axis=0, tiled=True)


def enter(here, down_hbm, tok_hbm, gain_hbm, wg_hbm, wu_hbm, last_hbm, wide, last, own, out, narrow, tok, gain, wg, wu, ready, sems):
    rows = own.shape[0]
    source = tok_hbm.at[pl.ds(pl.multiple_of(here[0] // 2 * rows, rows), rows)]
    halves = 2
    tokens = tok.shape[0] // halves
    cuts = [pl.ds(h * tokens, tokens) for h in range(halves)]
    pairs = ((down_hbm, narrow), (wg_hbm, wg), (wu_hbm, wu), (gain_hbm, gain), *[(tok_hbm.at[c], tok.at[c]) for c in cuts],
             (last_hbm, last), (source, own))
    pending = [pltpu.make_async_copy(a, b, sems.at[k]) for k, (a, b) in enumerate(pairs)]
    for c in pending:
        c.start()
    pending[0].wait()
    wide[...] = narrow[...].astype(F32)
    for c in pending[1:4]:
        c.wait()
    peers = ready.shape[0] // halves
    sent = []
    for h in range(halves):
        pending[4 + h].wait()
        front(tok.at[cuts[h]], gain, wg, wu, ready.at[pl.ds(h * peers, peers)])
        sent.append(pltpu.make_async_copy(ready.at[pl.ds(h * peers, peers)], out.at[pl.ds(h * peers, peers)], sems.at[len(pairs) + h]))
        sent[h].start()
    for c in pending[4 + halves :] + sent:
        c.wait()


def order(here, hid, out):
    quad = here[0] // 8 % 2 * 2 + here[0] % 2
    for k in range(out.shape[0]):
        for j in range(hid.shape[0]):
            held = hid.shape[2]
            out[k, j * held : (j + 1) * held] = hid[j, quad ^ k].astype(BF16)


def front(tok, gain, wg, wu, out):
    n_cb, _, lanes = out.shape
    rows, cols = tok.shape
    units = wg.shape[0]
    share = rows // n_cb
    half = share // 2
    first = lanes - units
    x = tok[...].astype(F32)
    sq = jnp.sum(x * x, axis=1, keepdims=True)
    scaled = (x * gain[...].astype(F32).reshape(1, cols)).astype(BF16)
    up = wu[...].astype(F32)
    left = jnp.concatenate([wg[...].astype(F32), up[:first]], axis=0).astype(BF16)
    gap = jnp.zeros((lanes // 2 - (units - first), cols), F32)
    none = jnp.zeros((lanes // 2, cols), F32)
    low = jnp.concatenate([up[first:], gap, none], axis=0).astype(BF16)
    high = jnp.concatenate([none, up[first:], gap], axis=0).astype(BF16)
    main = lax.dot_general(scaled, left, NT, preferred_element_type=F32)
    blocks = scaled.reshape(n_cb, 2, half, cols)
    sums = sq.reshape(n_cb, 2, half, 1)
    lane = lax.broadcasted_iota(jnp.int32, (n_cb * half, lanes), 1)
    rest = lax.dot_general(blocks[:, 0].reshape(n_cb * half, cols), low, NT, preferred_element_type=F32)
    rest = rest + lax.dot_general(blocks[:, 1].reshape(n_cb * half, cols), high, NT, preferred_element_type=F32)
    rest = jnp.where(lane == units - first, sums[:, 0].reshape(n_cb * half, 1), rest)
    rest = jnp.where(lane == lanes // 2 + units - first, sums[:, 1].reshape(n_cb * half, 1), rest)
    for j in range(n_cb):
        out[j, :share] = main[j * share : (j + 1) * share]
        out[j, share:] = rest[j * half : (j + 1) * half]


def middle(parts, out):
    n_cb, n_z0, n_y0, held, units = out.shape
    lanes = parts.shape[2]
    share = held * n_z0 * n_y0
    first = lanes - units
    total = parts[0]
    for k in range(1, n_cb):
        total = total + parts[k]
    main, rest = total[:share], total[share:]
    rest = jnp.concatenate([rest[:, : lanes // 2], rest[:, lanes // 2 :]], axis=0)
    inv = lax.rsqrt(rest[:, units - first : units - first + 1] / D + EPS)
    g = main[:, :units] * inv
    u = jnp.concatenate([main[:, units:], rest[:, : units - first]], axis=1) * inv
    hidden = (g / (1.0 + jnp.exp(-g)) * u).astype(BF16).astype(F32)
    r = 4
    n_yq = held // r
    for a in range(n_z0):
        for b in range(n_y0):
            rows = [((a * n_yq + q) * n_y0 + b) * r for q in range(n_yq)]
            block = jnp.concatenate([hidden[s : s + r] for s in rows], axis=0)
            for j in range(n_cb):
                out[j, a, b] = block


def back(hid, w0, w1, w2, w3, out):
    acc = None
    for k, w in enumerate((w0, w1, w2, w3)):
        part = jnp.dot(hid[k], w[...].astype(BF16), preferred_element_type=F32)
        acc = part if acc is None else acc + part
    n, held, lanes = out.shape
    blocks = acc.shape[1] // lanes
    per = held // blocks
    for k in range(n):
        out[k] = jnp.concatenate([acc[k * per : (k + 1) * per, b * lanes : (b + 1) * lanes] for b in range(blocks)], axis=0)


def fold(here, sums, residual, gain, gained, sq):
    per, cols = gained.shape
    pair = residual[...].astype(F32)
    down = jnp.sum(sums[...], axis=0)
    down = jnp.concatenate([down[b * per : (b + 1) * per] for b in range(down.shape[0] // per)], axis=1)
    value = 0.1 * jnp.where(here[0] % 2 == 1, pair[per:], pair[:per]) + down
    gained[...] = value * gain[...].astype(F32).reshape(1, cols)
    total = jnp.sum(value * value, axis=1, keepdims=True)
    sq[...] = jnp.broadcast_to(total[None], sq.shape)


def finish(gained, sq, out):
    total = jnp.sum(sq[...], axis=0)[:, :1]
    out[...] = (gained[...] * lax.rsqrt(total / D + EPS)).astype(BF16)


def body(tokens, norm_gain, w_gate, w_up, w_down, out_gain):
    n_cb = lax.axis_size("cb")
    n_quad = lax.axis_size(QUAD)
    n_rest = lax.axis_size(REST)
    rows, cols = tokens.shape
    units = w_gate.shape[1]
    own = rows // lax.axis_size(RA)
    share = rows // n_cb
    held = share // n_quad

    here = lax.axis_index(RA).astype(jnp.int32)[None]
    lanes = 128
    packed = share + share // 2
    inputs = (w_down, tokens, norm_gain, w_gate.T, w_up.T, out_gain)
    hbm = [pltpu.with_memory_space_constraint(x, pltpu.HBM) for x in inputs]
    whole = lambda *shape: pl.BlockSpec(shape, lambda i, m: (0,) * len(shape))
    mine, out_gain, residual, partial = pl.pallas_call(
        enter,
        grid_spec=pltpu.PrefetchScalarGridSpec(
            num_scalar_prefetch=1, grid=(1,), in_specs=[pl.BlockSpec(memory_space=pltpu.HBM)] * 6,
            out_specs=[whole(units, cols), whole(cols), whole(2 * own, cols), pl.BlockSpec(memory_space=pltpu.HBM)],
            scratch_shapes=[pltpu.VMEM((units, cols), BF16), pltpu.VMEM((rows, cols), BF16), pltpu.VMEM((cols,), BF16),
                            pltpu.VMEM((units, cols), BF16), pltpu.VMEM((units, cols), BF16), pltpu.VMEM((n_cb, packed, lanes), F32),
                            pltpu.SemaphoreType.DMA((10,))]),
        out_shape=[jax.ShapeDtypeStruct((units, cols), F32), jax.ShapeDtypeStruct((cols,), BF16), jax.ShapeDtypeStruct((2 * own, cols), BF16),
                   jax.ShapeDtypeStruct((n_cb, packed, lanes), F32)],
        name="enter", compiler_params=SMALL)(here, *hbm)
    others = []
    for k in range(1, n_quad):
        others.append(lax.ppermute(mine, QUAD, [(i, i ^ k) for i in range(n_quad)]))

    parts = exchange(partial, "cb")
    blocks = pl.pallas_call(middle, out_shape=jax.ShapeDtypeStruct((n_cb, 2, 2, held, units), F32), name="middle", compiler_params=SMALL)(parts)
    got = exchange(blocks.reshape(n_quad * n_cb, held, units), ("cb",) + QUAD)

    hidden = pl.pallas_call(
        order,
        grid_spec=pltpu.PrefetchScalarGridSpec(
            num_scalar_prefetch=1, grid=(1,), in_specs=[pl.BlockSpec((n_cb, n_quad, held, units), lambda i, m: (0, 0, 0, 0))],
            out_specs=pl.BlockSpec((n_quad, n_cb * held, units), lambda i, m: (0, 0, 0))),
        out_shape=jax.ShapeDtypeStruct((n_quad, n_cb * held, units), BF16), name="order", compiler_params=SMALL)(
        here, got.reshape(n_cb, n_quad, held, units))
    sums = pl.pallas_call(back, out_shape=jax.ShapeDtypeStruct((n_rest, own * cols // 128, 128), F32), name="back", compiler_params=SMALL)(
        hidden, mine, *others)
    sums = exchange(sums, REST)

    gained, sq = pl.pallas_call(
        fold,
        grid_spec=pltpu.PrefetchScalarGridSpec(
            num_scalar_prefetch=1, grid=(1,), in_specs=[
                pl.BlockSpec((n_rest, own * cols // 128, 128), lambda i, m: (0, 0, 0)), pl.BlockSpec((2 * own, cols), lambda i, m: (0, 0)),
                pl.BlockSpec((cols,), lambda i, m: (0,))],
            out_specs=[pl.BlockSpec((own, cols), lambda i, m: (0, 0)), pl.BlockSpec((n_cb, own, 128), lambda i, m: (0, 0, 0))]),
        out_shape=[jax.ShapeDtypeStruct((own, cols), F32), jax.ShapeDtypeStruct((n_cb, own, 128), F32)], name="fold", compiler_params=SMALL)(
        here, sums, residual, out_gain)
    sq = exchange(sq, "cb")
    return pl.pallas_call(finish, out_shape=jax.ShapeDtypeStruct((own, cols), BF16), name="finish", compiler_params=SMALL)(gained, sq)


def solution(mesh):
    finer = Mesh(mesh.devices.reshape(8, 2, 4, 2, mesh.shape["cb"]), (*RA, "cb"))
    placed = (P(None, "cb"), P("cb"), P("cb", RA), P("cb", RA), P(RA, "cb"), P("cb"))
    return jax.shard_map(body, mesh=finer, in_specs=placed, out_specs=P(RA, "cb"), check_vma=False)
```
